32 devices in a mesh: ep: 8 (over z, core), tp: 4 (over y, x).
Axes of the slice: x: 2, y: 2, z: 4, core: 2. Of those that a mesh axis runs over, the one named last changes fastest.
Arguments:
- token_rows: bfloat16 [192, 2048], P('ep', 'tp'), may hold values from -6 to 6
- prior_state: float32 [192, 64, 2048], P('ep', None, 'tp'), may hold values from -4 to 4
- first_gain: bfloat16 [2048], replicated, may hold values from 0.099609375 to 1.8984375
- w_recept: bfloat16 [2048, 2048], P(None, 'tp'), may hold values from -0.125 to 0.125
- w_key: bfloat16 [2048, 2048], P(None, 'tp'), may hold values from -0.125 to 0.125
- w_value: bfloat16 [2048, 2048], P(None, 'tp'), may hold values from -0.125 to 0.125
- decay_down: bfloat16 [2048, 96], P('tp'), may hold values from -0.125 to 0.125
- decay_up: bfloat16 [96, 2048], P(None, 'tp'), may hold values from -0.625 to 0.625
- decay_base: float32 [2048], P('tp'), may hold values from -4 to 3
- iclr_down: bfloat16 [2048, 96], P('tp'), may hold values from -0.125 to 0.125
- iclr_up: bfloat16 [96, 2048], P(None, 'tp'), may hold values from -0.625 to 0.625
- iclr_base: float32 [2048], P('tp'), may hold values from -4 to 4
- key_scale: bfloat16 [2048], P('tp'), may hold values from 0.29882812 to 1.5
- key_mix: bfloat16 [2048], P('tp'), may hold values from 0 to 2
- head_gain: bfloat16 [2048], P('tp'), may hold values from 0.099609375 to 1.8984375
- w_out: bfloat16 [2048, 2048], P(None, 'tp'), may hold values from -0.125 to 0.125
- second_gain: bfloat16 [2048], replicated, may hold values from 0.099609375 to 1.8984375
- routes: int32 [192, 4], P('ep'), may hold values from 0 to 7, all different within a row; in each aligned block of 24 rows (0 to 23, 24 to 47, ...) at most 18 rows name the same one
- route_weights: float32 [192, 4], P('ep'), may hold values from 0.2 to 1
- exp_gate: bfloat16 [8, 2048, 2048], P('ep', None, 'tp'), may hold values from -0.125 to 0.125
- exp_up: bfloat16 [8, 2048, 2048], P('ep', None, 'tp'), may hold values from -0.125 to 0.125
- exp_down: bfloat16 [8, 2048, 2048], P('ep', 'tp'), may hold values from -0.125 to 0.125
- dense_gate: bfloat16 [2048, 512], P(None, 'tp'), may hold values from -0.125 to 0.125
- dense_up: bfloat16 [2048, 512], P(None, 'tp'), may hold values from -0.125 to 0.125
- dense_down: bfloat16 [512, 2048], P('tp'), may hold values from -0.25 to 0.25
- dense_mix: bfloat16 [2048], replicated, may hold values from -0.125 to 0.125
Outputs:
- layer_out: bfloat16 [192, 2048], P('ep', 'tp')
- next_state: float32 [192, 64, 2048], P('ep', None, 'tp')
The draws below stay inside these ranges and needn't reach their ends.
Inputs may be any that keep to these rules, and one draw needn't show every extreme that they name: `routes`: each row names 4 different experts. Among the rows of one index of ep no expert is named by more than 18 rows, and in every draw some expert is named by exactly 18 of them.
All inputs are finite; a program needn't handle non-finite values.
Results may differ from the reference program's by a relative error of at most 0.018.
Values may be sent and summed in bfloat16 or wider, within the bound.
A program may use at most 64 MiB of HBM per device.

```python
import math
import jax
import jax.numpy as jnp
import numpy as np
from jax import lax

HEADS = 32
HEAD = 64
D = 2048
LR = 96
FF = 2048
DFF = 512
EXPERTS = 8
TOPK = 4
SEQ = 24
CAP = 18
BATCH = 192
N_TP = 4


def shard_levels(key, extent, shards, least, top_value):
    def one(dim, shards_of):
        heights = jax.random.uniform(jax.random.fold_in(jax.random.fold_in(key, 6), dim), (shards_of,), jnp.float32, least / len(shards), top_value / len(shards))
        return jnp.repeat(jnp.exp(heights), extent[dim] // shards_of).reshape((-1,) + (1,) * (len(extent) - dim - 1))

    factor_of = one(*shards[0])
    for cut in shards[1:]:
        factor_of = factor_of * one(*cut)
    return factor_of


def routed_block(rng, own, number, rows, number_of, top, limit, lean):
    sequence = jax.random.permutation(rng, number_of)
    crowded, common = shares(number_of, rows * top, limit, lean, True), shares(number_of, rows * top, limit, lean, False)
    places = jnp.arange(number_of)

    def named(sizes, rotation):
        used = int((sizes > 0).sum())
        fixed = max(1, used // 4)
        shifted = fixed + (places - fixed + rotation * (used - fixed)) % max(1, number_of - fixed)
        return jnp.zeros((number_of,), jnp.int32).at[sequence[jnp.where(places < fixed, places, shifted)]].set(jnp.asarray(sizes, jnp.int32))

    sizes = jnp.where(number % 4 == 0, named(crowded, number // 4), named(common, number - number // 4 - 1))
    mixed = jax.random.permutation(jax.random.fold_in(own, 3), number_of)
    donor, taker = mixed[0:number_of // 2 * 2:2], mixed[1:number_of // 2 * 2:2]
    slack = jnp.minimum(sizes[donor] - 1, limit - sizes[taker]) // 2
    slack = jnp.where((donor == sequence[0]) | (taker == sequence[0]) | (sizes[taker] == 0), 0, jnp.maximum(slack, 0))
    shifted = jax.random.randint(jax.random.fold_in(own, 4), (number_of // 2,), 0, 1 << 20) % (slack + 1)
    sizes = sizes.at[donor].add(-shifted).at[taker].add(shifted)
    labels = jnp.searchsorted(jnp.cumsum(sizes), jnp.arange(rows * top), side="right").astype(jnp.int32)
    table = labels.reshape(top, rows).T
    table = table[jax.random.permutation(jax.random.fold_in(own, 1), rows)]
    rotation = jax.random.randint(jax.random.fold_in(own, 2), (rows, 1), 0, top)
    return jnp.take_along_axis(table, (jnp.arange(top)[None, :] + rotation) % top, axis=1)


def shares(count, total, limit, skew, full):
    loads = [(1 << 20) // math.isqrt(standing ** skew) + 1 for standing in range(1, count + 1)]
    largest = limit if full else min(limit, max(-(-total // count), total * loads[0] // sum(loads)))
    least = 1 if total - largest >= count - 1 else 0
    given, surplus = [largest] + [least] * (count - 1), total - largest - least * (count - 1)
    while surplus > 0:
        movable = [i for i in range(1, count) if given[i] < largest] or [i for i in range(1, count) if given[i] < limit]
        pool, budget = sum([loads[i] for i in movable]), surplus
        for i in movable:
            extra = min(limit - given[i], max(1, budget * loads[i] // pool), surplus)
            given[i] = given[i] + extra
            surplus = surplus - extra
    return np.array(given)


def scatter_about(rng, extent, width, reach, cuts=(), kind=jnp.bfloat16):
    drawn = width * jax.random.normal(rng, extent, jnp.float32)
    if cuts:
        drawn = drawn * shard_levels(rng, extent, cuts, -0.22, 0.18)
    return jnp.clip(drawn, -reach, reach).astype(kind)


def setup_inputs(seed: int = 0) -> dict:
    arg_keys = jax.random.split(jax.random.key(seed), 27)
    token_rows = scatter_about(arg_keys[0], (BATCH, D), 1.0, 6.0, ((0, 8), (1, 4)))
    prior_state = scatter_about(arg_keys[1], (BATCH, HEAD, D), 0.5, 4.0, ((0, 8), (2, 4)), jnp.float32)
    first_gain = jnp.clip(1.0 + 0.18 * jax.random.normal(arg_keys[2], (D,), jnp.float32), 0.099609375, 1.8984375).astype(jnp.bfloat16)
    w_recept = scatter_about(arg_keys[3], (D, D), D ** -0.5, 0.125, ((1, 4),))
    w_key = scatter_about(arg_keys[4], (D, D), D ** -0.5, 0.125, ((1, 4),))
    w_value = scatter_about(arg_keys[5], (D, D), D ** -0.5, 0.125, ((1, 4),))
    decay_down = scatter_about(arg_keys[6], (D, LR), D ** -0.5, 0.125, ((0, 4),))
    decay_up = scatter_about(arg_keys[7], (LR, D), LR ** -0.5, 0.625, ((1, 4),))
    decay_base = jnp.clip(-4.0 + 7.0 * jax.random.uniform(arg_keys[8], (D,), jnp.float32) ** shard_levels(arg_keys[8], (D,), ((0, 4),), -0.2, 0.2), -4.0, 3.0)
    iclr_down = scatter_about(arg_keys[9], (D, LR), D ** -0.5, 0.125, ((0, 4),))
    iclr_up = scatter_about(arg_keys[10], (LR, D), LR ** -0.5, 0.625, ((1, 4),))
    iclr_base = scatter_about(arg_keys[11], (D,), 1.0, 4.0, ((0, 4),), jnp.float32)
    key_scale = jnp.clip(0.29882812 + 1.2011719 * jax.random.uniform(arg_keys[12], (D,), jnp.float32) ** shard_levels(arg_keys[12], (D,), ((0, 4),), -0.2, 0.2), 0.29882812, 1.5).astype(jnp.bfloat16)
    key_mix = jnp.clip(2.0 * jax.random.uniform(arg_keys[13], (D,), jnp.float32) ** shard_levels(arg_keys[13], (D,), ((0, 4),), -0.2, 0.2), 0.0, 2.0).astype(jnp.bfloat16)
    head_gain = jnp.clip(1.0 + 0.18 * jax.random.normal(arg_keys[14], (D,), jnp.float32), 0.099609375, 1.8984375).astype(jnp.bfloat16)
    w_out = scatter_about(arg_keys[15], (D, D), D ** -0.5, 0.125, ((1, 4),))
    second_gain = jnp.clip(1.0 + 0.18 * jax.random.normal(arg_keys[16], (D,), jnp.float32), 0.099609375, 1.8984375).astype(jnp.bfloat16)
    routes_keys = jax.random.split(jax.random.fold_in(arg_keys[17], 1), BATCH // SEQ)
    routes_turns = jax.random.permutation(jax.random.fold_in(arg_keys[17], 3), BATCH // SEQ)
    routes = jax.vmap(lambda own, number: routed_block(jax.random.fold_in(arg_keys[17], 2), own, number, SEQ, EXPERTS, TOPK, CAP, 2))(routes_keys, routes_turns).reshape((BATCH, TOPK))
    route_weights = jnp.clip(0.2 + 0.8 * jax.random.uniform(arg_keys[18], (BATCH, TOPK), jnp.float32) ** shard_levels(arg_keys[18], (BATCH, TOPK), ((0, 8),), -0.2, 0.2), 0.2, 1.0)
    exp_gate = scatter_about(arg_keys[19], (EXPERTS, D, FF), D ** -0.5, 0.125, ((0, 8), (2, 4)))
    exp_up = scatter_about(arg_keys[20], (EXPERTS, D, FF), D ** -0.5, 0.125, ((0, 8), (2, 4)))
    exp_down = scatter_about(arg_keys[21], (EXPERTS, FF, D), FF ** -0.5, 0.125, ((0, 8), (1, 4)))
    dense_gate = scatter_about(arg_keys[22], (D, DFF), D ** -0.5, 0.125, ((1, 4),))
    dense_up = scatter_about(arg_keys[23], (D, DFF), D ** -0.5, 0.125, ((1, 4),))
    dense_down = scatter_about(arg_keys[24], (DFF, D), DFF ** -0.5, 0.25, ((0, 4),))
    dense_mix = scatter_about(arg_keys[25], (D,), D ** -0.5, 0.125)
    return dict(token_rows=token_rows, prior_state=prior_state, first_gain=first_gain, w_recept=w_recept, w_key=w_key, w_value=w_value, decay_down=decay_down, decay_up=decay_up, decay_base=decay_base, iclr_down=iclr_down, iclr_up=iclr_up, iclr_base=iclr_base, key_scale=key_scale, key_mix=key_mix, head_gain=head_gain, w_out=w_out, second_gain=second_gain, routes=routes, route_weights=route_weights, exp_gate=exp_gate, exp_up=exp_up, exp_down=exp_down, dense_gate=dense_gate, dense_up=dense_up, dense_down=dense_down, dense_mix=dense_mix)


def norm_rows(values, gain):
    floats = values.astype(jnp.float32)
    mean_square = lax.optimization_barrier(jnp.mean(floats * floats, axis=1, keepdims=True))
    return (floats * lax.rsqrt(mean_square + 1e-06) * gain.astype(jnp.float32)).astype(jnp.bfloat16)

def product(left, right):
    return jnp.dot(left, right, preferred_element_type=jnp.float32)

def group_slots(group_routes):
    flat_ids = group_routes.reshape(SEQ * TOPK)
    onehot = (flat_ids[:, None] == jnp.arange(EXPERTS, dtype=jnp.int32)[None, :]).astype(jnp.float32)
    earlier = (jnp.arange(SEQ * TOPK)[:, None] > jnp.arange(SEQ * TOPK)[None, :]).astype(jnp.float32)
    before = jnp.dot(earlier, onehot, precision=lax.Precision.HIGHEST)
    ranking = lax.optimization_barrier(jnp.sum(before * onehot, axis=1)).astype(jnp.int32)
    return flat_ids * CAP + ranking

def one_expert(operands):
    expert_rows, gate_mat, up_mat, down_mat = operands
    hidden = (jax.nn.silu(product(expert_rows, gate_mat)) * product(expert_rows, up_mat)).astype(jnp.bfloat16)
    block = FF // N_TP
    partial_value = jnp.einsum('rjf,jfd->rjd', hidden.reshape(-1, N_TP, block).astype(jnp.float32), down_mat.reshape(N_TP, block, D).astype(jnp.float32), precision=lax.Precision.HIGHEST).astype(jnp.bfloat16)
    partial_value = lax.optimization_barrier(partial_value)
    return lax.optimization_barrier(jnp.sum(partial_value.astype(jnp.float32), axis=1)).astype(jnp.bfloat16)

def reference(token_rows, prior_state, first_gain, w_recept, w_key, w_value, decay_down, decay_up, decay_base, iclr_down, iclr_up, iclr_base, key_scale, key_mix, head_gain, w_out, second_gain, routes, route_weights, exp_gate, exp_up, exp_down, dense_gate, dense_up, dense_down, dense_mix):
    first = norm_rows(token_rows, first_gain)
    recept = product(first, w_recept).astype(jnp.bfloat16)
    key_rows = product(first, w_key).astype(jnp.bfloat16)
    value_rows = product(first, w_value).astype(jnp.bfloat16)
    decay_act = jnp.tanh(product(first, decay_down)).astype(jnp.bfloat16)
    rate_act = product(first, iclr_down).astype(jnp.bfloat16)
    decay_rate = jnp.exp(-jnp.exp(-jax.nn.softplus(-(decay_base + product(decay_act, decay_up))) - 0.5))
    iclr_rate = jax.nn.sigmoid(iclr_base + product(rate_act, iclr_up))
    key_float = key_rows.astype(jnp.float32)
    scaled = (key_float * key_scale.astype(jnp.float32)).reshape(BATCH, HEADS, HEAD)
    removal = scaled * lax.rsqrt(lax.optimization_barrier(jnp.sum(scaled * scaled, axis=-1, keepdims=True)) + 1e-06)
    written = (key_float * (1.0 + (iclr_rate - 1.0) * key_mix.astype(jnp.float32))).reshape(BATCH, HEADS, HEAD)
    state_grid = prior_state.reshape(BATCH, HEAD, HEADS, HEAD)
    recall = lax.optimization_barrier(jnp.sum(state_grid * removal[:, None], axis=-1))
    scaled_removal = removal * iclr_rate.reshape(BATCH, HEADS, HEAD)
    value_cols = jnp.transpose(value_rows.astype(jnp.float32).reshape(BATCH, HEADS, HEAD), (0, 2, 1))
    state_grid = state_grid * decay_rate.reshape(BATCH, 1, HEADS, HEAD) - recall[..., None] * scaled_removal[:, None] + value_cols[..., None] * written[:, None]
    read = lax.optimization_barrier(jnp.sum(state_grid * recept.astype(jnp.float32).reshape(BATCH, 1, HEADS, HEAD), axis=-1))
    read = jnp.transpose(read, (0, 2, 1))
    centered = read - lax.optimization_barrier(jnp.mean(read, axis=-1, keepdims=True))
    variance = lax.optimization_barrier(jnp.mean(centered * centered, axis=-1, keepdims=True))
    head_out = centered * lax.rsqrt(variance + 0.00064) * head_gain.astype(jnp.float32).reshape(HEADS, HEAD)
    head_out = head_out.reshape(BATCH, D).astype(jnp.bfloat16)
    mixer_out = product(head_out, w_out).astype(jnp.bfloat16)
    residual = (token_rows.astype(jnp.float32) + mixer_out.astype(jnp.float32)).astype(jnp.bfloat16)
    second = norm_rows(residual, second_gain)
    groups = BATCH // SEQ
    token_of = jnp.repeat(jnp.arange(SEQ, dtype=jnp.int32), TOPK)
    slot_index = jax.vmap(group_slots)(routes.reshape(groups, SEQ, TOPK))

    def group_table(slots_one):
        return jnp.full((EXPERTS * CAP,), SEQ, jnp.int32).at[slots_one].set(token_of)
    slot_table = jax.vmap(group_table)(slot_index)
    padded = jnp.concatenate([second.reshape(groups, SEQ, D), jnp.zeros((groups, 1, D), jnp.bfloat16)], axis=1)

    def take_rows(source, indices):
        return jnp.take(source, indices, axis=0)
    buffers = jax.vmap(take_rows)(padded, slot_table)
    by_expert = jnp.transpose(buffers.reshape(groups, EXPERTS, CAP, D), (1, 0, 2, 3)).reshape(EXPERTS, groups * CAP, D)
    results = lax.map(one_expert, (by_expert, exp_gate, exp_up, exp_down))
    returned = jnp.transpose(results.reshape(EXPERTS, groups, CAP, D), (1, 0, 2, 3)).reshape(groups, EXPERTS * CAP, D)
    picked = jax.vmap(take_rows)(returned, slot_index).astype(jnp.float32)
    weighted = picked * route_weights.reshape(groups, SEQ * TOPK)[..., None]
    routed = lax.optimization_barrier(jnp.sum(weighted.reshape(groups, SEQ, TOPK, D), axis=2)).reshape(BATCH, D)
    dense_hidden = (jax.nn.silu(product(second, dense_gate)) * product(second, dense_up)).astype(jnp.bfloat16)
    dense_out = product(dense_hidden, dense_down)
    mix_gate = jax.nn.sigmoid(product(second, dense_mix[:, None])[:, 0])
    layer_out = (residual.astype(jnp.float32) + routed + mix_gate[:, None] * dense_out).astype(jnp.bfloat16)
    return (layer_out, state_grid.reshape(BATCH, HEAD, D))
```

```python
import functools

import jax
import jax.numpy as jnp
from jax import lax
from jax.experimental import pallas as pl
from jax.experimental.pallas import tpu as pltpu
from jax.sharding import PartitionSpec as P

HEAD = 64
CORES = 2
GROUP = 8
norm_eps = 1e-06
head_eps = 0.00064
key_eps = 1e-06
F32 = jnp.float32
BF16 = jnp.bfloat16


def product(left, right):
    return jnp.dot(left, right, preferred_element_type=F32)


def kernel(
    tp, ep,
    x_ref, gains, vecs, routes, rweights,
    state_h, wr_h, wk_h, wv_h, dd_h, id_h, du_h, iu_h, wo_h, eg_h, eu_h, ed_h, dg_h, dup_h, ddn_h,
    out_ref, ns_h,
    st, wr, wk, wv, dd, idn, du, iu, wo, eg, eu, ed, dg, dup, ddn,
    xg, pbuf, pg, wbuf, wg, hbuf, hg, rbuf, grid, dbuf, drecv,
    rem_s, dr_s, val_s, dec_s, srem_s, wri_s, rec_s, q_s, rb,
    norm_s, mine_s, psend, precv, hsum, hrecv, qbuf, qrecv,
    lsem, ssem, rsem,
):
    nz = ep // CORES
    t = lax.axis_index("tp")
    e = lax.axis_index("ep")
    z = e // CORES
    core = lax.rem(e, CORES)
    mate = 1 - core
    S, W = x_ref.shape
    D = W * tp
    L = dd.shape[1]

    loads = {}
    pairs = [("dd", dd_h, dd), ("id", id_h, idn), ("wr", wr_h, wr), ("wk", wk_h, wk), ("wv", wv_h, wv),
             ("du", du_h, du), ("iu", iu_h, iu), ("st", state_h, st), ("wo", wo_h, wo),
             ("dg", dg_h, dg), ("dup", dup_h, dup), ("ddn", ddn_h, ddn),
             ("eg", eg_h.at[0], eg), ("eu", eu_h.at[0], eu), ("ed", ed_h.at[0], ed)]
    for i, (name, src, dst) in enumerate(pairs):
        loads[name] = pltpu.make_async_copy(src, dst, lsem.at[i])
        loads[name].start()
    next_copy = pltpu.make_async_copy(st, ns_h, lsem.at[len(pairs)])

    barrier = pltpu.get_barrier_semaphore()
    for d in range(1, tp):
        pl.semaphore_signal(barrier, inc=1, device_id={"ep": e, "tp": lax.rem(t + d, tp)},
                            device_id_type=pl.DeviceIdType.MESH)
    for d in range(1, ep):
        pl.semaphore_signal(barrier, inc=1, device_id={"ep": lax.rem(e + d, ep), "tp": t},
                            device_id_type=pl.DeviceIdType.MESH)
    pl.semaphore_wait(barrier, tp - 1 + ep - 1)

    sent = []

    def send(src, dst, dev_e, dev_t):
        i = len(sent)
        c = pltpu.make_async_remote_copy(
            src_ref=src, dst_ref=dst, send_sem=ssem.at[i], recv_sem=rsem.at[i],
            device_id={"ep": dev_e, "tp": dev_t}, device_id_type=pl.DeviceIdType.MESH)
        c.start()
        sent.append(c)
        return c

    def to_tp(src, dst):
        return [send(src, dst, e, lax.rem(t + d, tp)) for d in range(1, tp)]

    def all_cols(block):
        return jnp.concatenate([block(k) for k in range(tp)], axis=-1)

    xc = to_tp(x_ref, xg.at[t])
    xg[t] = x_ref[...]

    lane = lax.broadcasted_iota(jnp.int32, (S, 128), 1)
    wmat = jnp.zeros((S, 128), F32)
    for k in range(routes.shape[1]):
        wmat += jnp.where(lane == routes[:, k:k + 1], rweights[:, k:k + 1], 0.0)
    wbuf[...] = wmat
    wg[e] = wmat
    wc = [send(wbuf, wg.at[e], lax.rem(e + d, ep), t) for d in range(1, ep)]

    own = pl.ds(pl.multiple_of(t * W, 128), W)
    x_own = x_ref[...].astype(F32)
    xs = (x_own * gains[0:1, own]).astype(BF16)
    loads["dd"].wait()
    loads["id"].wait()
    pbuf[:, :L] = product(xs, dd[...])
    pbuf[:, 128:128 + L] = product(xs, idn[...])
    pg[t] = pbuf[...]
    pc = to_tp(pbuf, pg.at[t])

    C = min(256, W)
    ri = lax.broadcasted_iota(jnp.int32, (C, C), 0) // HEAD
    ci = lax.broadcasted_iota(jnp.int32, (C, C), 1) // HEAD
    ones = (ri == ci).astype(F32).astype(BF16)

    def seg(v):
        hi = v.astype(BF16)
        lo = (v - hi.astype(F32)).astype(BF16)
        return jnp.concatenate(
            [product(hi[:, c:c + C], ones) + product(lo[:, c:c + C], ones) for c in range(0, W, C)], axis=1)

    for c in xc:
        c.wait_recv()
    full = all_cols(lambda k: xg[k].astype(F32))
    inv = lax.rsqrt(jnp.mean(full * full, axis=1, keepdims=True) + norm_eps)
    first = (full * inv * gains[0:1, :]).astype(BF16)
    loads["wk"].wait()
    key = product(first, wk[...]).astype(BF16).astype(F32)
    loads["wr"].wait()
    recept = product(first, wr[...]).astype(BF16).astype(F32)
    loads["wv"].wait()
    value = product(first, wv[...]).astype(BF16).astype(F32)
    for c in pc:
        c.wait_recv()
    low = pg[0]
    for k in range(1, tp):
        low += pg[k]
    low = low * inv
    loads["du"].wait()
    loads["iu"].wait()
    decay_pre = vecs[0:1, :] + product(jnp.tanh(low[:, :L]).astype(BF16), du[...])
    decay = jnp.exp(-0.6065306597126334 * jax.nn.sigmoid(decay_pre))
    rate = jax.nn.sigmoid(vecs[1:2, :] + product(low[:, 128:128 + L].astype(BF16), iu[...]))
    scaled = key * vecs[2:3, :]
    removal = scaled * lax.rsqrt(seg(scaled * scaled) + key_eps)
    written = key * (1.0 + (rate - 1.0) * vecs[3:4, :])
    srem = removal * rate
    rem_s[...] = removal
    dr_s[...] = decay * recept
    val_s[...] = value
    dec_s[...] = decay
    srem_s[...] = srem
    wri_s[...] = written
    bonus_a = seg(srem * recept)
    bonus_b = seg(written * recept)

    eye = (lax.broadcasted_iota(jnp.int32, (HEAD, C), 0)
           == lax.rem(lax.broadcasted_iota(jnp.int32, (HEAD, C), 1), HEAD)).astype(F32)
    loads["st"].wait()

    def read_group(g, carry):
        for c in range(0, W, C):
            cols = slice(c, c + C)
            parts = []
            for k in range(GROUP):
                s = g * GROUP + k
                parts.append((st[s, :, cols] * rem_s[pl.ds(s, 1), cols]).astype(BF16))
            for k in range(GROUP):
                s = g * GROUP + k
                parts.append((st[s, :, cols] * dr_s[pl.ds(s, 1), cols]).astype(BF16))
            both = product(jnp.concatenate(parts, axis=0), ones)
            for k in range(GROUP):
                s = g * GROUP + k
                a = both[k * HEAD:(k + 1) * HEAD]
                rb[s, :, cols] = a
                rec_s[pl.ds(s, 1), cols] = jnp.sum(a * eye, axis=0, keepdims=True)
                b = both[(GROUP + k) * HEAD:(GROUP + k + 1) * HEAD]
                q_s[pl.ds(s, 1), cols] = jnp.sum(b * eye, axis=0, keepdims=True)
        return carry

    lax.fori_loop(0, S // GROUP, read_group, 0)
    read = q_s[...] - rec_s[...] * bonus_a + value * bonus_b
    cent = read - seg(read) * (1.0 / HEAD)
    var = seg(cent * cent) * (1.0 / HEAD)
    head = (cent * lax.rsqrt(var + head_eps) * vecs[4:5, :]).astype(BF16)
    hbuf[...] = head
    hg[t] = head
    hc = to_tp(hbuf, hg.at[t])

    def next_group(g, carry):
        for c in range(0, W, C):
            cols = slice(c, c + C)
            parts = []
            for k in range(GROUP):
                s = g * GROUP + k
                parts.append((eye * val_s[pl.ds(s, 1), cols]).astype(BF16))
            vals = product(jnp.concatenate(parts, axis=0), ones)
            for k in range(GROUP):
                s = g * GROUP + k
                st[s, :, cols] = (st[s, :, cols] * dec_s[pl.ds(s, 1), cols]
                                  - rb[s, :, cols] * srem_s[pl.ds(s, 1), cols]
                                  + vals[k * HEAD:(k + 1) * HEAD] * wri_s[pl.ds(s, 1), cols])
        return carry

    lax.fori_loop(0, S // GROUP, next_group, 0)
    next_copy.start()

    for c in hc:
        c.wait_recv()
    loads["wo"].wait()
    mixer = product(all_cols(lambda k: hg[k]), wo[...]).astype(BF16)
    residual = (x_own + mixer.astype(F32)).astype(BF16)
    rbuf[...] = residual
    grid[core, z, t] = residual

    tc = to_tp(rbuf, grid.at[core, z, t])
    zc = [send(rbuf, grid.at[core, z, t], lax.rem(z + d, nz) * CORES + core, t) for d in range(1, nz)]
    fc = []
    for d in range(1, nz):
        zc[d - 1].wait_recv()
        zz = lax.rem(z - d + nz, nz)
        fc.append(to_tp(grid.at[core, zz, t], grid.at[core, zz, t]))
    for c in tc:
        c.wait_recv()
    mc = [send(grid.at[core, z], grid.at[core, z], z * CORES + mate, t)]

    def normed(rows):
        scale = lax.rsqrt(jnp.mean(rows * rows, axis=-1, keepdims=True) + norm_eps)
        return rows * scale * gains[1:2, :]

    second = normed(all_cols(lambda k: grid[core, z, k].astype(F32))).astype(BF16)
    for n in ("dg", "dup", "ddn"):
        loads[n].wait()
    dhid = (jax.nn.silu(product(second, dg[...])) * product(second, dup[...])).astype(BF16)
    dpart = product(dhid, ddn[...])
    for k in range(tp):
        dbuf[k] = dpart[:, k * W:(k + 1) * W].astype(BF16)
    dc = [send(dbuf.at[lax.rem(t + d, tp)], drecv.at[d - 1], e, lax.rem(t + d, tp)) for d in range(1, tp)]
    mix = jax.nn.sigmoid(jnp.sum(second.astype(F32) * gains[2:3, :], axis=1, keepdims=True))

    for d in range(1, nz):
        for c in fc[d - 1]:
            c.wait_recv()
        zz = lax.rem(z - d + nz, nz)
        mc.append(send(grid.at[core, zz], grid.at[core, zz], z * CORES + mate, t))
    for c in mc:
        c.wait_recv()
    for k in range(nz):
        rows = jnp.concatenate(
            [all_cols(lambda j, i=i: grid[i, k, j].astype(F32)) for i in range(CORES)], axis=0)
        norm_s[k * CORES * S:(k + 1) * CORES * S, :] = normed(rows).astype(BF16)

    for c in wc:
        c.wait_recv()
    wall = wg[...].reshape(ep * S, 128)
    wcol = jnp.sum(jnp.where(lax.broadcasted_iota(jnp.int32, (ep * S, 128), 1) == e, wall, 0.0),
                   axis=1, keepdims=True)
    loads["eg"].wait()
    gate = product(norm_s[...], eg[...])
    loads["eu"].wait()
    hidden = (jax.nn.silu(gate) * product(norm_s[...], eu[...])).astype(BF16)
    loads["ed"].wait()
    upper = core.astype(F32)
    order = list(range(1, tp)) + [0]
    rc = []
    for d in order:
        c = lax.rem(t + d, tp)
        part = product(hidden, ed[:, pl.ds(pl.multiple_of(c * W, 128), W)]) * wcol
        part = part.reshape(nz, CORES, S, W)
        psend[d] = (part[:, 0] * upper + part[:, 1] * (1.0 - upper)).astype(BF16)
        mine_s[d] = part[:, 1] * upper + part[:, 0] * (1.0 - upper)
        rc.append(send(psend.at[d], precv.at[d], z * CORES + mate, t))
    sc = []
    for i, d in enumerate(order):
        rc[i].wait_recv()
        both = mine_s[d] + precv[d].astype(F32)
        if d:
            hsum[d - 1] = both.astype(BF16)
            sc.append(send(hsum.at[d - 1], hrecv.at[d - 1], e, lax.rem(t + d, tp)))
        else:
            total = both
    for d in range(1, tp):
        sc[d - 1].wait_recv()
        total += hrecv[d - 1].astype(F32)
    qbuf[...] = total.astype(BF16)
    qc = [send(qbuf.at[lax.rem(z + d, nz)], qrecv.at[d - 1], lax.rem(z + d, nz) * CORES + core, t)
          for d in range(1, nz)]
    for c in dc:
        c.wait_recv()
    dense = dbuf[t].astype(F32)
    for d in range(1, tp):
        dense += drecv[d - 1].astype(F32)
    acc = residual.astype(F32) + mix * dense + qbuf[z].astype(F32)
    for d in range(1, nz):
        qc[d - 1].wait_recv()
        acc += qrecv[d - 1].astype(F32)
    out_ref[...] = acc.astype(BF16)
    next_copy.wait()
    for c in sent:
        c.wait_send()


def local(
    tp, ep, token_rows, prior_state, first_gain, w_recept, w_key, w_value, decay_down, decay_up, decay_base,
    iclr_down, iclr_up, iclr_base, key_scale, key_mix, head_gain, w_out, second_gain, routes, route_weights,
    exp_gate, exp_up, exp_down, dense_gate, dense_up, dense_down, dense_mix,
):
    S, W = token_rows.shape
    D = W * tp
    nz = ep // CORES
    gains = jnp.stack([first_gain, second_gain, dense_mix]).astype(F32)
    vecs = jnp.stack([decay_base, iclr_base, key_scale.astype(F32), key_mix.astype(F32), head_gain.astype(F32)])
    big = [prior_state, w_recept, w_key, w_value, decay_down, iclr_down, decay_up, iclr_up, w_out,
           exp_gate, exp_up, exp_down, dense_gate, dense_up, dense_down]
    V = lambda a: pltpu.VMEM(a.shape, a.dtype)
    E = lambda a: pltpu.VMEM(a.shape[1:], a.dtype)
    copies = (4 * (tp - 1) + (ep - 1) + 2 * (nz - 1) + (nz - 1) * (tp - 1) + nz + 2 * (tp - 1) + tp)
    row = pltpu.VMEM((S, W), F32)
    scratch = [
        V(prior_state), V(w_recept), V(w_key), V(w_value), V(decay_down), V(iclr_down), V(decay_up), V(iclr_up),
        V(w_out), E(exp_gate), E(exp_up), E(exp_down), V(dense_gate), V(dense_up), V(dense_down),
        pltpu.VMEM((tp, S, W), BF16), pltpu.VMEM((S, 256), F32), pltpu.VMEM((tp, S, 256), F32),
        pltpu.VMEM((S, 128), F32), pltpu.VMEM((ep, S, 128), F32),
        pltpu.VMEM((S, W), BF16), pltpu.VMEM((tp, S, W), BF16), pltpu.VMEM((S, W), BF16),
        pltpu.VMEM((CORES, nz, tp, S, W), BF16), pltpu.VMEM((tp, S, W), BF16), pltpu.VMEM((tp - 1, S, W), BF16),
        row, row, row, row, row, row, row, row, V(prior_state),
        pltpu.VMEM((ep * S, D), BF16), pltpu.VMEM((tp, nz, S, W), F32), pltpu.VMEM((tp, nz, S, W), BF16),
        pltpu.VMEM((tp, nz, S, W), BF16), pltpu.VMEM((tp - 1, nz, S, W), BF16),
        pltpu.VMEM((tp - 1, nz, S, W), BF16), pltpu.VMEM((nz, S, W), BF16), pltpu.VMEM((nz - 1, S, W), BF16),
        pltpu.SemaphoreType.DMA((len(big) + 1,)), pltpu.SemaphoreType.DMA((copies,)),
        pltpu.SemaphoreType.DMA((copies,)),
    ]
    vm = pl.BlockSpec(memory_space=pltpu.VMEM)
    anym = pl.BlockSpec(memory_space=pl.ANY)
    return pl.pallas_call(
        functools.partial(kernel, tp, ep),
        name="layer",
        out_shape=(jax.ShapeDtypeStruct((S, W), BF16), jax.ShapeDtypeStruct(prior_state.shape, F32)),
        in_specs=[vm] * 5 + [anym] * len(big),
        out_specs=(vm, anym),
        scratch_shapes=scratch,
        compiler_params=pltpu.CompilerParams(
            collective_id=0, has_side_effects=True, vmem_limit_bytes=63 * 1024 * 1024),
    )(token_rows, gains, vecs, routes, route_weights, *big)


def solution(mesh):
    in_specs = (
        P("ep", "tp"), P("ep", None, "tp"), P(), P(None, "tp"), P(None, "tp"), P(None, "tp"), P("tp", None),
        P(None, "tp"), P("tp"), P("tp", None), P(None, "tp"), P("tp"), P("tp"), P("tp"), P("tp"), P(None, "tp"),
        P(), P("ep", None), P("ep", None), P("ep", None, "tp"), P("ep", None, "tp"), P("ep", "tp", None),
        P(None, "tp"), P(None, "tp"), P("tp", None), P(),
    )
    out_specs = (P("ep", "tp"), P("ep", None, "tp"))
    body = functools.partial(local, mesh.shape["tp"], mesh.shape["ep"])
    return jax.shard_map(body, mesh=mesh, in_specs=in_specs, out_specs=out_specs, check_vma=False)
```

```python
import functools

import jax
import jax.numpy as jnp
from jax import lax
from jax.experimental import pallas as pl
from jax.experimental.pallas import tpu as pltpu
from jax.sharding import PartitionSpec as P

HEAD = 64
CORES = 2
GROUP = 8
VMEM_BYTES = 67043328
norm_eps = 1e-06
head_eps = 0.00064
key_eps = 1e-06
F32 = jnp.float32
BF16 = jnp.bfloat16


def product(left, right):
    return jnp.dot(left, right, preferred_element_type=F32)


def product_t(left, right):
    return lax.dot_general(left, right, (((1,), (1,)), ((), ())), preferred_element_type=F32)


def kernel(
    tp, ep,
    x_ref, fg_ref, sg_ref, dm_ref, db_ref, ib_ref, ks_ref, km_ref, hgain_ref, routes, rweights,
    state_h, wr_h, wk_h, wv_h, dd_h, id_h, du_h, iu_h, wo_h, eg_h, eu_h, ed_h, dg_h, dup_h, ddn_h,
    out_ref, ns_h,
    st, wr, wk, wv, dd, idn, du, iu, wo, eg, eu, ed, dg, dup, ddn,
    xg, pbuf, pg, wbuf, wg, hbuf, hg, rbuf, grid, dbuf, drecv,
    rem_s, dr_s, val_s, dec_s, srem_s, wri_s, rec_s, q_s, rb,
    norm_s, mine_s, psend, precv, hsum, hrecv, qbuf, qrecv,
    lsem, ssem, rsem,
):
    nz = ep // CORES
    t = lax.axis_index("tp")
    e = lax.axis_index("ep")
    z = e // CORES
    core = lax.rem(e, CORES)
    mate = 1 - core
    S, W = x_ref.shape
    D = W * tp
    L = dd.shape[0]

    def line(ref):
        return ref[...].astype(F32).reshape(1, -1)

    loads = {}
    pairs = [("dd", dd_h, dd), ("id", id_h, idn), ("wr", wr_h, wr), ("wk", wk_h, wk), ("wv", wv_h, wv),
             ("du", du_h, du), ("iu", iu_h, iu), ("st", state_h, st), ("wo", wo_h, wo),
             ("dg", dg_h, dg), ("dup", dup_h, dup), ("ddn", ddn_h, ddn),
             ("eg", eg_h.at[0], eg), ("eu", eu_h.at[0], eu), ("ed", ed_h.at[0], ed)]
    for i, (name, src, dst) in enumerate(pairs):
        loads[name] = pltpu.make_async_copy(src, dst, lsem.at[i])
        loads[name].start()

    barrier = pltpu.get_barrier_semaphore()
    for d in range(1, tp):
        pl.semaphore_signal(barrier, inc=1, device_id={"ep": e, "tp": lax.rem(t + d, tp)},
                            device_id_type=pl.DeviceIdType.MESH)
    for d in range(1, ep):
        pl.semaphore_signal(barrier, inc=1, device_id={"ep": lax.rem(e + d, ep), "tp": t},
                            device_id_type=pl.DeviceIdType.MESH)
    pl.semaphore_wait(barrier, tp - 1 + ep - 1)

    sent = []

    def send(src, dst, dev_e, dev_t):
        i = len(sent)
        c = pltpu.make_async_remote_copy(
            src_ref=src, dst_ref=dst, send_sem=ssem.at[i], recv_sem=rsem.at[i],
            device_id={"ep": dev_e, "tp": dev_t}, device_id_type=pl.DeviceIdType.MESH)
        c.start()
        sent.append(c)
        return c

    def to_tp(src, dst):
        return [send(src, dst, e, lax.rem(t + d, tp)) for d in range(1, tp)]

    def all_cols(block):
        return jnp.concatenate([block(k) for k in range(tp)], axis=-1)

    xc = to_tp(x_ref, xg.at[t])
    xg[t] = x_ref[...]

    expert = lax.broadcasted_iota(jnp.int32, (128, S), 0)
    wide = jnp.zeros((128, S), F32)
    for k in range(routes.shape[0]):
        wide += jnp.where(expert == routes[k:k + 1, :], rweights[k:k + 1, :], 0.0)
    same = (lax.broadcasted_iota(jnp.int32, (S, S), 0) == lax.broadcasted_iota(jnp.int32, (S, S), 1)).astype(F32)
    wmat = lax.dot_general(same, wide, (((1,), (1,)), ((), ())), precision=lax.Precision.HIGHEST,
                           preferred_element_type=F32)
    wbuf[...] = wmat
    wg[e] = wmat
    wc = [send(wbuf, wg.at[e], lax.rem(e + d, ep), t) for d in range(1, ep)]

    own = pl.ds(pl.multiple_of(t * W, 128), W)
    x_own = x_ref[...].astype(F32)
    first_gain = line(fg_ref)
    own_gain = first_gain[:, :W]
    for k in range(1, tp):
        own_gain = jnp.where(t == k, first_gain[:, k * W:(k + 1) * W], own_gain)
    xs = (x_own * own_gain).astype(BF16)
    loads["dd"].wait()
    loads["id"].wait()
    pbuf[:, :L] = product_t(xs, dd[...])
    pbuf[:, 128:128 + L] = product_t(xs, idn[...])
    pg[t] = pbuf[...]
    pc = to_tp(pbuf, pg.at[t])

    C = min(256, W)
    ri = lax.broadcasted_iota(jnp.int32, (C, C), 0) // HEAD
    ci = lax.broadcasted_iota(jnp.int32, (C, C), 1) // HEAD
    ones = (ri == ci).astype(F32).astype(BF16)

    def seg(v):
        hi = v.astype(BF16)
        lo = (v - hi.astype(F32)).astype(BF16)
        return jnp.concatenate(
            [product(hi[:, c:c + C], ones) + product(lo[:, c:c + C], ones) for c in range(0, W, C)], axis=1)

    for c in xc:
        c.wait_recv()
    full = all_cols(lambda k: xg[k].astype(F32))
    inv = lax.rsqrt(jnp.mean(full * full, axis=1, keepdims=True) + norm_eps)
    first = (full * inv * first_gain).astype(BF16)
    loads["wk"].wait()
    key = product(first, wk[...]).astype(BF16).astype(F32)
    loads["wr"].wait()
    recept = product(first, wr[...]).astype(BF16).astype(F32)
    loads["wv"].wait()
    value = product(first, wv[...]).astype(BF16).astype(F32)
    for c in pc:
        c.wait_recv()
    low = pg[0]
    for k in range(1, tp):
        low += pg[k]
    low = low * inv
    loads["du"].wait()
    loads["iu"].wait()
    decay_pre = line(db_ref) + product(jnp.tanh(low[:, :L]).astype(BF16), du[...])
    decay = jnp.exp(-0.6065306597126334 * jax.nn.sigmoid(decay_pre))
    rate = jax.nn.sigmoid(line(ib_ref) + product(low[:, 128:128 + L].astype(BF16), iu[...]))
    scaled = key * line(ks_ref)
    removal = scaled * lax.rsqrt(seg(scaled * scaled) + key_eps)
    written = key * (1.0 + (rate - 1.0) * line(km_ref))
    srem = removal * rate
    rem_s[...] = removal
    dr_s[...] = decay * recept
    val_s[...] = value
    dec_s[...] = decay
    srem_s[...] = srem
    wri_s[...] = written
    bonus_a = seg(srem * recept)
    bonus_b = seg(written * recept)

    eye = (lax.broadcasted_iota(jnp.int32, (HEAD, C), 0)
           == lax.rem(lax.broadcasted_iota(jnp.int32, (HEAD, C), 1), HEAD)).astype(F32)
    loads["st"].wait()

    def read_group(g, carry):
        for c in range(0, W, C):
            cols = slice(c, c + C)
            parts = []
            for k in range(GROUP):
                s = g * GROUP + k
                parts.append((st[s, :, cols] * rem_s[pl.ds(s, 1), cols]).astype(BF16))
            for k in range(GROUP):
                s = g * GROUP + k
                parts.append((st[s, :, cols] * dr_s[pl.ds(s, 1), cols]).astype(BF16))
            both = product(jnp.concatenate(parts, axis=0), ones)
            for k in range(GROUP):
                s = g * GROUP + k
                a = both[k * HEAD:(k + 1) * HEAD]
                rb[s, :, cols] = a
                rec_s[pl.ds(s, 1), cols] = jnp.sum(a * eye, axis=0, keepdims=True)
                b = both[(GROUP + k) * HEAD:(GROUP + k + 1) * HEAD]
                q_s[pl.ds(s, 1), cols] = jnp.sum(b * eye, axis=0, keepdims=True)
        return carry

    lax.fori_loop(0, S // GROUP, read_group, 0)
    read = q_s[...] - rec_s[...] * bonus_a + value * bonus_b
    cent = read - seg(read) * (1.0 / HEAD)
    var = seg(cent * cent) * (1.0 / HEAD)
    head = (cent * lax.rsqrt(var + head_eps) * line(hgain_ref)).astype(BF16)
    hbuf[...] = head
    hg[t] = head
    hc = to_tp(hbuf, hg.at[t])

    def next_group(g, carry):
        for c in range(0, W, C):
            cols = slice(c, c + C)
            parts = []
            for k in range(GROUP):
                s = g * GROUP + k
                parts.append((eye * val_s[pl.ds(s, 1), cols]).astype(BF16))
            vals = product(jnp.concatenate(parts, axis=0), ones)
            for k in range(GROUP):
                s = g * GROUP + k
                ns_h[s, :, cols] = (st[s, :, cols] * dec_s[pl.ds(s, 1), cols]
                                  - rb[s, :, cols] * srem_s[pl.ds(s, 1), cols]
                                  + vals[k * HEAD:(k + 1) * HEAD] * wri_s[pl.ds(s, 1), cols])
        return carry

    next_group(0, 0)

    for c in hc:
        c.wait_recv()
    loads["wo"].wait()
    mixer = product(all_cols(lambda k: hg[k]), wo[...]).astype(BF16)
    residual = (x_own + mixer.astype(F32)).astype(BF16)
    rbuf[...] = residual
    grid[core, z, t] = residual

    tc = to_tp(rbuf, grid.at[core, z, t])
    zc = [send(rbuf, grid.at[core, z, t], lax.rem(z + d, nz) * CORES + core, t) for d in range(1, nz)]
    fc = []
    for d in range(1, nz):
        zc[d - 1].wait_recv()
        zz = lax.rem(z - d + nz, nz)
        fc.append(to_tp(grid.at[core, zz, t], grid.at[core, zz, t]))
    for c in tc:
        c.wait_recv()
    mc = [send(grid.at[core, z], grid.at[core, z], z * CORES + mate, t)]

    second_gain = line(sg_ref)

    def normed(rows):
        scale = lax.rsqrt(jnp.mean(rows * rows, axis=-1, keepdims=True) + norm_eps)
        return rows * scale * second_gain

    second = normed(all_cols(lambda k: grid[core, z, k].astype(F32))).astype(BF16)
    for n in ("dg", "dup", "ddn"):
        loads[n].wait()
    dhid = (jax.nn.silu(product(second, dg[...])) * product(second, dup[...])).astype(BF16)
    dpart = product(dhid, ddn[...])
    for k in range(tp):
        dbuf[k] = dpart[:, k * W:(k + 1) * W].astype(BF16)
    dc = [send(dbuf.at[lax.rem(t + d, tp)], drecv.at[d - 1], e, lax.rem(t + d, tp)) for d in range(1, tp)]
    mix = jax.nn.sigmoid(jnp.sum(second.astype(F32) * line(dm_ref), axis=1, keepdims=True))

    for d in range(1, nz):
        for c in fc[d - 1]:
            c.wait_recv()
        zz = lax.rem(z - d + nz, nz)
        mc.append(send(grid.at[core, zz], grid.at[core, zz], z * CORES + mate, t))
    for d in range(nz):
        mc[d].wait_recv()
        zz = lax.rem(z - d + nz, nz)
        rows = jnp.concatenate(
            [all_cols(lambda j, i=i: grid[i, zz, j].astype(F32)) for i in range(CORES)], axis=0)
        norm_s[pl.ds(pl.multiple_of(zz * CORES * S, 16), CORES * S), :] = normed(rows).astype(BF16)

    for c in wc:
        c.wait_recv()
    wall = wg[...].reshape(ep * S, 128)
    wcol = jnp.sum(jnp.where(lax.broadcasted_iota(jnp.int32, (ep * S, 128), 1) == e, wall, 0.0),
                   axis=1, keepdims=True)
    loads["eg"].wait()
    gate = product(norm_s[...], eg[...])
    loads["eu"].wait()
    hidden = (jax.nn.silu(gate) * product(norm_s[...], eu[...])).astype(BF16)
    loads["ed"].wait()
    upper = core.astype(F32)
    order = list(range(1, tp)) + [0]
    rc = []
    for d in order:
        c = lax.rem(t + d, tp)
        part = product(hidden, ed[:, pl.ds(pl.multiple_of(c * W, 128), W)]) * wcol
        part = part.reshape(nz, CORES, S, W)
        psend[d] = (part[:, 0] * upper + part[:, 1] * (1.0 - upper)).astype(BF16)
        mine_s[d] = part[:, 1] * upper + part[:, 0] * (1.0 - upper)
        rc.append(send(psend.at[d], precv.at[d], z * CORES + mate, t))
    sc = []
    for i, d in enumerate(order):
        rc[i].wait_recv()
        both = mine_s[d] + precv[d].astype(F32)
        if d:
            hsum[d - 1] = both.astype(BF16)
            sc.append(send(hsum.at[d - 1], hrecv.at[d - 1], e, lax.rem(t + d, tp)))
        else:
            total = both
    lax.fori_loop(1, S // GROUP, next_group, 0)
    for d in range(1, tp):
        sc[d - 1].wait_recv()
        total += hrecv[d - 1].astype(F32)
    qbuf[...] = total.astype(BF16)
    qc = [send(qbuf.at[lax.rem(z + d, nz)], qrecv.at[d - 1], lax.rem(z + d, nz) * CORES + core, t)
          for d in range(1, nz)]
    for c in dc:
        c.wait_recv()
    dense = dbuf[t].astype(F32)
    for d in range(1, tp):
        dense += drecv[d - 1].astype(F32)
    acc = residual.astype(F32) + mix * dense + qbuf[z].astype(F32)
    for d in range(1, nz):
        qc[d - 1].wait_recv()
        acc += qrecv[d - 1].astype(F32)
    out_ref[...] = acc.astype(BF16)
    for c in sent:
        c.wait_send()


def local(
    tp, ep, token_rows, prior_state, first_gain, w_recept, w_key, w_value, decay_down, decay_up, decay_base,
    iclr_down, iclr_up, iclr_base, key_scale, key_mix, head_gain, w_out, second_gain, routes, route_weights,
    exp_gate, exp_up, exp_down, dense_gate, dense_up, dense_down, dense_mix,
):
    S, W = token_rows.shape
    D = W * tp
    nz = ep // CORES
    decay_down, iclr_down = decay_down.T, iclr_down.T
    small = [token_rows, first_gain, second_gain, dense_mix, decay_base, iclr_base, key_scale, key_mix, head_gain,
             routes.T, route_weights.T]
    big = [prior_state, w_recept, w_key, w_value, decay_down, iclr_down, decay_up, iclr_up, w_out,
           exp_gate, exp_up, exp_down, dense_gate, dense_up, dense_down]
    V = lambda a: pltpu.VMEM(a.shape, a.dtype)
    E = lambda a: pltpu.VMEM(a.shape[1:], a.dtype)
    copies = (4 * (tp - 1) + (ep - 1) + 2 * (nz - 1) + (nz - 1) * (tp - 1) + nz + 2 * (tp - 1) + tp)
    room = pl.cdiv(4 * prior_state.size + 2 * token_rows.size, 8192) * 8192
    row = pltpu.VMEM((S, W), F32)
    scratch = [
        V(prior_state), V(w_recept), V(w_key), V(w_value), V(decay_down), V(iclr_down), V(decay_up), V(iclr_up),
        V(w_out), E(exp_gate), E(exp_up), E(exp_down), V(dense_gate), V(dense_up), V(dense_down),
        pltpu.VMEM((tp, S, W), BF16), pltpu.VMEM((S, 256), F32), pltpu.VMEM((tp, S, 256), F32),
        pltpu.VMEM((S, 128), F32), pltpu.VMEM((ep, S, 128), F32),
        pltpu.VMEM((S, W), BF16), pltpu.VMEM((tp, S, W), BF16), pltpu.VMEM((S, W), BF16),
        pltpu.VMEM((CORES, nz, tp, S, W), BF16), pltpu.VMEM((tp, S, W), BF16), pltpu.VMEM((tp - 1, S, W), BF16),
        row, row, row, row, row, row, row, row, V(prior_state),
        pltpu.VMEM((ep * S, D), BF16), pltpu.VMEM((tp, nz, S, W), F32), pltpu.VMEM((tp, nz, S, W), BF16),
        pltpu.VMEM((tp, nz, S, W), BF16), pltpu.VMEM((tp - 1, nz, S, W), BF16),
        pltpu.VMEM((tp - 1, nz, S, W), BF16), pltpu.VMEM((nz, S, W), BF16), pltpu.VMEM((nz - 1, S, W), BF16),
        pltpu.SemaphoreType.DMA((len(big),)), pltpu.SemaphoreType.DMA((copies,)),
        pltpu.SemaphoreType.DMA((copies,)),
    ]
    vm = pl.BlockSpec(memory_space=pltpu.VMEM)
    anym = pl.BlockSpec(memory_space=pltpu.HBM)
    return pl.pallas_call(
        functools.partial(kernel, tp, ep),
        name="layer",
        out_shape=(pltpu.VMEM((S, W), BF16), pltpu.VMEM(prior_state.shape, F32)),
        in_specs=[vm] * len(small) + [anym] * len(big),
        out_specs=(vm, vm),
        scratch_shapes=scratch,
        compiler_params=pltpu.CompilerParams(
            collective_id=0, has_side_effects=True, vmem_limit_bytes=VMEM_BYTES - room),
    )(*small, *big)


def solution(mesh):
    in_specs = (
        P("ep", "tp"), P("ep", None, "tp"), P(), P(None, "tp"), P(None, "tp"), P(None, "tp"), P("tp", None),
        P(None, "tp"), P("tp"), P("tp", None), P(None, "tp"), P("tp"), P("tp"), P("tp"), P("tp"), P(None, "tp"),
        P(), P("ep", None), P("ep", None), P("ep", None, "tp"), P("ep", None, "tp"), P("ep", "tp", None),
        P(None, "tp"), P(None, "tp"), P("tp", None), P(),
    )
    out_specs = (P("ep", "tp"), P("ep", None, "tp"))
    body = functools.partial(local, mesh.shape["tp"], mesh.shape["ep"])
    return jax.shard_map(body, mesh=mesh, in_specs=in_specs, out_specs=out_specs, check_vma=False)
```
